32 devices in a mesh: sp: 16 (over z, y, x), tp: 2 (over core).
Axes of the slice: x: 2, y: 2, z: 4, core: 2. Of those that a mesh axis runs over, the one named last changes fastest.
Arguments:
- queries: bfloat16 [8192, 2048], P('sp', 'tp'), may hold values from -14 to 14
- key_states: bfloat16 [8192, 512], P('sp', 'tp'), may hold values from -14 to 14
- value_states: bfloat16 [8192, 512], P('sp', 'tp'), may hold values from -6 to 6
- sink_logits: float32 [32], P('tp'), may hold values from 0 to 5
- out_weight: bfloat16 [2048, 2048], P('tp'), may hold values from -0.125 to 0.125
- residual: bfloat16 [8192, 2048], P(('sp', 'tp')), may hold values from -6 to 6
- gain_attn: float32 [2048], replicated, may hold values from 0.1 to 1.9
- gain_before: float32 [2048], replicated, may hold values from 0.1 to 1.9
- gain_after: float32 [2048], replicated, may hold values from 0.1 to 1.9
- gate_weight: bfloat16 [2048, 5632], P('sp', 'tp'), may hold values from -0.125 to 0.125
- value_weight: bfloat16 [2048, 5632], P('sp', 'tp'), may hold values from -0.125 to 0.125
- gate_taps: float32 [3, 5632], P(None, 'tp'), may hold values from -3 to 3
- value_taps: float32 [3, 5632], P(None, 'tp'), may hold values from -3 to 3
- down_weight: bfloat16 [5632, 2048], P('tp', 'sp'), may hold values from -0.078125 to 0.078125
Outputs:
- layer_out: bfloat16 [8192, 2048], P(('sp', 'tp'))
The draws below stay inside these ranges and needn't reach their ends.
All inputs are finite; a program needn't handle non-finite values.
Results may differ from the reference program's by a relative error of at most 0.018.
Values may be sent and summed in bfloat16 or wider, within the bound.
A program may use at most 128 MiB of HBM per device.

```python
import jax
import jax.numpy as jnp
from jax import lax

D = 2048
HQ = 32
KV = 8
HD = 64
FF = 5632
WINDOW = 128
CONVK = 3
TOKENS = 8192
N_TP = 2


def drawn_keys(key):
    base = jax.random.truncated_normal(jax.random.fold_in(key, 11), -2.5, 2.5, (TOKENS, KV * HD), jnp.float32)
    return base


def draw_key_states(key, part):
    base = drawn_keys(key)
    return base.astype(jnp.bfloat16)


def draw_queries(key, part):
    own = jax.random.truncated_normal(jax.random.fold_in(key, 21), -2.5, 2.5, (TOKENS, HQ * HD), jnp.float32)
    return own.astype(jnp.bfloat16)


def block_scale(key, shape, cuts, smallest, high):
    loudness, own = 1.0, jax.random.fold_in(key, 6)
    for axis_at, blocks in cuts:
        steps = jnp.exp(jax.random.uniform(jax.random.fold_in(own, axis_at), (blocks,), jnp.float32, smallest / len(cuts), high / len(cuts)))
        loudness = loudness * jnp.repeat(steps, shape[axis_at] // blocks).reshape([-1 if axis == axis_at else 1 for axis in range(len(shape))])
    return loudness


def scatter_about(rng, extent, scale, most, shards=(), kind=jnp.bfloat16):
    loudness = block_scale(rng, extent, shards, -0.22, 0.18) if shards else 1.0
    drawn = jax.random.normal(rng, extent, jnp.float32) * scale * loudness
    return jnp.minimum(jnp.maximum(drawn, -most), most).astype(kind)


def setup_inputs(seed: int = 0) -> dict:
    arg_keys = jax.random.split(jax.random.key(seed), 15)
    return {
        "queries": draw_queries(jax.random.fold_in(arg_keys[14], 71), 0),
        "key_states": draw_key_states(jax.random.fold_in(arg_keys[14], 71), 0),
        "value_states": scatter_about(arg_keys[2], (TOKENS, KV * HD), 1.0, 6.0, ((0, 16), (1, 2))),
        "sink_logits": jnp.clip(5.0 * jax.random.uniform(arg_keys[3], (HQ,), jnp.float32) ** block_scale(arg_keys[3], (HQ,), ((0, 2),), -0.2, 0.2), 0.0, 5.0),
        "out_weight": scatter_about(arg_keys[4], (HQ * HD, D), (HQ * HD) ** -0.5, 0.125, ((0, 2),)),
        "residual": scatter_about(arg_keys[5], (TOKENS, D), 1.0, 6.0, ((0, 32),)),
        "gain_attn": jnp.clip(1.0 + 0.18 * jax.random.normal(arg_keys[6], (D,), jnp.float32), 0.1, 1.9),
        "gain_before": jnp.clip(1.0 + 0.18 * jax.random.normal(arg_keys[7], (D,), jnp.float32), 0.1, 1.9),
        "gain_after": jnp.clip(1.0 + 0.18 * jax.random.normal(arg_keys[8], (D,), jnp.float32), 0.1, 1.9),
        "gate_weight": scatter_about(arg_keys[9], (D, FF), D ** -0.5, 0.125, ((0, 16), (1, 2))),
        "value_weight": scatter_about(arg_keys[10], (D, FF), D ** -0.5, 0.125, ((0, 16), (1, 2))),
        "gate_taps": scatter_about(arg_keys[11], (CONVK, FF), 0.577, 3.0, ((1, 2),), jnp.float32),
        "value_taps": scatter_about(arg_keys[12], (CONVK, FF), 0.577, 3.0, ((1, 2),), jnp.float32),
        "down_weight": scatter_about(arg_keys[13], (FF, D), FF ** -0.5, 0.078125, ((0, 2), (1, 16))),
    }


NEG_FILL = -1e+30

def rms_scale(matrix):
    return matrix * lax.rsqrt(lax.optimization_barrier(jnp.mean(matrix * matrix, axis=-1, keepdims=True)) + 1e-06)

def attention(queries, key_states, value_states, sink_logits):
    length = queries.shape[0]
    blocks = length // WINDOW
    grouping = HQ // KV
    zeros_rows = jnp.zeros((WINDOW, KV * HD), jnp.bfloat16)
    keys_ext = jnp.concatenate([zeros_rows, key_states], axis=0).reshape(blocks + 1, WINDOW, KV, HD)
    values_ext = jnp.concatenate([zeros_rows, value_states], axis=0).reshape(blocks + 1, WINDOW, KV, HD)
    key_blocks = jnp.concatenate([keys_ext[:-1], keys_ext[1:]], axis=1)
    value_blocks = jnp.concatenate([values_ext[:-1], values_ext[1:]], axis=1)
    query_blocks = queries.reshape(blocks, WINDOW, KV, grouping, HD)
    qpos = jnp.arange(length, dtype=jnp.int32).reshape(blocks, WINDOW)
    kpos = jnp.concatenate([qpos - WINDOW, qpos], axis=1)
    visible = (kpos[:, None, :] <= qpos[:, :, None]) & (qpos[:, :, None] - kpos[:, None, :] < WINDOW) & (kpos[:, None, :] >= 0)
    sinks_all = sink_logits.reshape(KV, grouping)

    def one_head(inputs):
        query_part, key_part, value_part, sink_part = inputs
        scores = jnp.einsum('nqgd,nkd->ngqk', query_part.astype(jnp.float32), key_part.astype(jnp.float32)) * HD ** (-0.5)
        scores = jnp.where(visible[:, None], scores, NEG_FILL)
        sink_col = sink_part[None, :, None]
        top = jnp.maximum(lax.optimization_barrier(jnp.max(scores, axis=-1)), sink_col)
        expo = jnp.exp(scores - top[..., None])
        total = lax.optimization_barrier(jnp.sum(expo, axis=-1)) + jnp.exp(sink_col - top)
        probs = (expo / total[..., None]).astype(jnp.bfloat16)
        result = jnp.einsum('ngqk,nkd->nqgd', probs.astype(jnp.float32), value_part.astype(jnp.float32))
        return result.astype(jnp.bfloat16)
    heads_out = lax.map(one_head, (jnp.moveaxis(query_blocks, 2, 0), jnp.moveaxis(key_blocks, 2, 0), jnp.moveaxis(value_blocks, 2, 0), sinks_all))
    return jnp.moveaxis(heads_out, 0, 2).reshape(length, HQ * HD)

def grouped_sum(left, right):
    width = left.shape[1] // N_TP
    total = jnp.zeros((left.shape[0], right.shape[1]), jnp.float32)
    for group_index in range(N_TP):
        part = jnp.dot(left[:, group_index * width:(group_index + 1) * width], right[group_index * width:(group_index + 1) * width], preferred_element_type=jnp.float32)
        total = total + part.astype(jnp.bfloat16).astype(jnp.float32)
    return total

def causal_taps(upward, kernel):
    length = upward.shape[0]
    padded = jnp.concatenate([jnp.zeros((CONVK - 1, upward.shape[1]), jnp.bfloat16), upward], axis=0).astype(jnp.float32)
    result = jnp.zeros((length, upward.shape[1]), jnp.float32)
    for tap_index in range(CONVK):
        result = result + kernel[tap_index][None, :] * padded[tap_index:tap_index + length]
    return result

def reference(queries, key_states, value_states, sink_logits, out_weight, residual, gain_attn, gain_before, gain_after, gate_weight, value_weight, gate_taps, value_taps, down_weight):
    attended = attention(queries, key_states, value_states, sink_logits)
    attn_proj = grouped_sum(attended, out_weight)
    middle = residual.astype(jnp.float32) + rms_scale(attn_proj) * gain_attn
    normed = (rms_scale(middle) * gain_before).astype(jnp.bfloat16)
    gate_up = jnp.dot(normed, gate_weight, preferred_element_type=jnp.float32).astype(jnp.bfloat16)
    value_up = jnp.dot(normed, value_weight, preferred_element_type=jnp.float32).astype(jnp.bfloat16)
    gate_conv = causal_taps(gate_up, gate_taps)
    value_conv = causal_taps(value_up, value_taps)
    hidden = (jax.nn.silu(gate_conv) * value_conv).astype(jnp.bfloat16)
    down = grouped_sum(hidden, down_weight)
    return (middle + rms_scale(down) * gain_after).astype(jnp.bfloat16)
```

```python
import functools

import jax
import jax.numpy as jnp
from jax import lax
from jax.experimental import pallas as pl
from jax.experimental.pallas import tpu as pltpu
from jax.sharding import PartitionSpec as P

HD = 64
WINDOW = 128
TEAM = 4


NEG_FILL = -1e30
MESH = pl.DeviceIdType.MESH
VMEM_BYTES = 60 * 1024 * 1024

def passed_along(block, axis, distance):
    devices = range(lax.axis_size(axis))
    route = [(i - distance, i) for i in devices if i - distance in devices]
    return lax.ppermute(block, axis, route)


def rms_scale(matrix):
    return matrix * lax.rsqrt(jnp.mean(matrix * matrix, axis=-1, keepdims=True) + 1e-06)


def attention_local(queries, key_states, value_states, sink_logits):
    length = queries.shape[0]
    blocks = length // WINDOW
    kv_local = key_states.shape[1] // HD
    grouping = queries.shape[1] // key_states.shape[1]
    earlier_keys, earlier_values = passed_along(
        (key_states[length - WINDOW :], value_states[length - WINDOW :]), "sp", 1
    )
    keys_ext = jnp.concatenate([earlier_keys, key_states], axis=0).reshape(
        blocks + 1, WINDOW, kv_local, HD
    )
    values_ext = jnp.concatenate([earlier_values, value_states], axis=0).reshape(
        blocks + 1, WINDOW, kv_local, HD
    )
    key_blocks = jnp.concatenate([keys_ext[:-1], keys_ext[1:]], axis=1)
    value_blocks = jnp.concatenate([values_ext[:-1], values_ext[1:]], axis=1)
    query_blocks = queries.reshape(blocks, WINDOW, kv_local, grouping, HD)
    offset = lax.axis_index("sp") * length
    qpos = (offset + jnp.arange(length, dtype=jnp.int32)).reshape(blocks, WINDOW)
    kpos = jnp.concatenate([qpos - WINDOW, qpos], axis=1)
    visible = (
        (kpos[:, None, :] <= qpos[:, :, None])
        & (qpos[:, :, None] - kpos[:, None, :] < WINDOW)
        & (kpos[:, None, :] >= 0)
    )
    scores = jnp.einsum(
        "nqhgd,nkhd->nhgqk", query_blocks, key_blocks, preferred_element_type=jnp.float32
    ) * HD ** (-0.5)
    scores = jnp.where(visible[:, None, None], scores, NEG_FILL)
    sink_col = sink_logits.reshape(kv_local, grouping)[None, :, :, None]
    top = jnp.maximum(jnp.max(scores, axis=-1), sink_col)
    expo = jnp.exp(scores - top[..., None])
    total = jnp.sum(expo, axis=-1) + jnp.exp(sink_col - top)
    probs = (expo / total[..., None]).astype(jnp.bfloat16)
    result = jnp.einsum(
        "nhgqk,nkhd->nqhgd", probs, value_blocks, preferred_element_type=jnp.float32
    )
    return result.astype(jnp.bfloat16).reshape(length, queries.shape[1])


def causal_local(upward, earlier, kernel):
    length = upward.shape[0]
    padded = jnp.concatenate([earlier, upward], axis=0).astype(jnp.float32)
    result = jnp.zeros(upward.shape, jnp.float32)
    for tap_index in range(kernel.shape[0]):
        result = result + kernel[tap_index][None, :] * padded[tap_index : tap_index + length]
    return result


def on_device_plain(
    queries,
    key_states,
    value_states,
    sink_logits,
    out_weight,
    residual,
    gain_attn,
    gain_before,
    gain_after,
    gate_weight,
    value_weight,
    gate_taps,
    value_taps,
    down_weight,
):
    length = queries.shape[0]
    attended = attention_local(queries, key_states, value_states, sink_logits)
    selected = attended
    attn_proj = lax.psum_scatter(
        jnp.dot(selected, out_weight, preferred_element_type=jnp.float32).astype(jnp.bfloat16),
        "tp",
        scatter_dimension=0,
        tiled=True,
    ).astype(jnp.float32)
    middle = residual.astype(jnp.float32) + rms_scale(attn_proj) * gain_attn
    normed = (rms_scale(middle) * gain_before).astype(jnp.bfloat16)
    whole_rows = lax.all_gather(normed, "tp", axis=0, tiled=True)
    gate_full, value_full = (
        lax.all_gather(gate_weight, "sp", axis=0, tiled=True),
        lax.all_gather(value_weight, "sp", axis=0, tiled=True),
    )
    gate_up = jnp.dot(whole_rows, gate_full, preferred_element_type=jnp.float32).astype(
        jnp.bfloat16
    )
    value_up = jnp.dot(whole_rows, value_full, preferred_element_type=jnp.float32).astype(
        jnp.bfloat16
    )
    reach = gate_taps.shape[0] - 1
    gate_before, value_before = passed_along(
        (gate_up[length - reach :], value_up[length - reach :]), "sp", 1
    )
    gate_conv = causal_local(gate_up, gate_before, gate_taps)
    value_conv = causal_local(value_up, value_before, value_taps)
    hidden = (jax.nn.silu(gate_conv) * value_conv).astype(jnp.bfloat16)
    down_whole = lax.all_gather(down_weight, "sp", axis=1, tiled=True)
    selected = hidden
    down = lax.psum_scatter(
        jnp.dot(selected, down_whole, preferred_element_type=jnp.float32).astype(jnp.bfloat16),
        "tp",
        scatter_dimension=0,
        tiled=True,
    ).astype(jnp.float32)
    return (middle + rms_scale(down) * gain_after).astype(jnp.bfloat16)


def team_peer(place, turn):
    low, high = place % 2, place // 2
    if turn & 1:
        low = 1 - low
    if turn & 2:
        high = 1 - high
    return high * 2 + low


def remote(src, dst, send, recv, **device):
    return pltpu.make_async_remote_copy(
        src_ref=src, dst_ref=dst, send_sem=send, recv_sem=recv, device_id=device, device_id_type=MESH
    )


def greet(devices):
    barrier = pltpu.get_barrier_semaphore()
    for device in devices:
        pl.semaphore_signal(barrier, inc=1, device_id=device, device_id_type=MESH)
    pl.semaphore_wait(barrier, len(devices))


def row_scale(block):
    return lax.rsqrt(jnp.mean(block * block, axis=-1, keepdims=True) + 1e-06)


def front_kernel(
    ring,
    q_ref,
    k_ref,
    v_ref,
    sink_ref,
    ow_ref,
    res_ref,
    ga_ref,
    gb_ref,
    gate_in,
    value_in,
    down_in,
    rows_all,
    gate_all,
    value_all,
    down_all,
    mid_ref,
    k_ext,
    v_ext,
    att,
    snd,
    rcv,
    own,
    nrm,
    halo_s,
    halo_r,
    trade_s,
    trade_r,
    local_sem,
    ring_s,
    ring_r,
    pair_s,
    pair_r,
    rows_s,
    rows_r,
    mate_s,
    mate_r,
):
    sp, tp = lax.axis_index("sp"), lax.axis_index("tp")
    members = ring * TEAM
    level, place = sp // TEAM, sp % TEAM
    up = (level + 1) % ring * TEAM + place
    down = (level + ring - 1) % ring * TEAM + place
    after, before = (sp + 1) % members, (sp + members - 1) % members
    mate = 1 - tp
    length = q_ref.shape[0]
    share = length // 2
    deep = gate_in.shape[1]
    units = gate_in.shape[2]
    wide = down_in.shape[1]
    sends = []

    greet(
        [{"sp": level * TEAM + team_peer(place, turn)} for turn in range(1, TEAM)]
        + [{"tp": mate}, {"sp": up}, {"sp": down}, {"sp": after}, {"sp": before}]
    )

    def begin(copy):
        copy.start()
        sends.append(copy)
        return copy

    halos = [
        begin(
            remote(
                ref.at[pl.ds(length - WINDOW, WINDOW)],
                ext.at[pl.ds(0, WINDOW)],
                halo_s.at[i],
                halo_r.at[i],
                sp=after,
            )
        )
        for i, (ref, ext) in enumerate(((k_ref, k_ext), (v_ref, v_ext)))
    ]

    def span(m, ref, start, size):
        if m < 2:
            return ref.at[pl.ds(pl.multiple_of(start * deep, deep), size * deep)]
        return ref.at[:, pl.ds(pl.multiple_of(start * wide, wide), size * wide)]

    def piece(m, member):
        if m < 2:
            return (gate_in, value_in)[m].at[member]
        return down_in.at[pl.ds(pl.multiple_of(member * units, units), units)]

    wholes = (gate_all, value_all, down_all)
    trades, locals_ = [], []
    for m in range(3):
        trades.append(
            [
                begin(
                    remote(
                        piece(m, team_peer(place, turn)),
                        span(m, wholes[m], sp, 1),
                        trade_s.at[m, turn - 1],
                        trade_r.at[m, turn - 1],
                        sp=level * TEAM + team_peer(place, turn),
                    )
                )
                for turn in (3, 1, 2)
            ]
        )
        copy = pltpu.make_async_copy(piece(m, place), span(m, wholes[m], sp, 1), local_sem.at[m])
        copy.start()
        locals_.append(copy)

    last = ring // 2
    ring_copies = {}

    def ring_start(m, step):
        if step == 1:
            locals_[m].wait()
            for copy in trades[m]:
                copy.wait_recv()
        for side, towards in ((0, up), (1, down)):
            if step > 1:
                ring_copies[m, step - 1, side].wait_recv()
            source = (level + ring - (step - 1)) % ring if side == 0 else (level + step - 1) % ring
            if step < last:
                block = span(m, wholes[m], source * TEAM, TEAM)
            else:
                block = span(m, wholes[m], source * TEAM + side * (TEAM // 2), TEAM // 2)
            sems = (ring_s.at[m, step - 1, side], ring_r.at[m, step - 1, side])
            ring_copies[m, step, side] = begin(remote(block, block, *sems, sp=towards))

    k_ext[pl.ds(WINDOW, length)] = k_ref[...]
    v_ext[pl.ds(WINDOW, length)] = v_ref[...]
    for copy in halos:
        copy.wait_recv()
    heads_kv = k_ref.shape[1] // HD
    grouping = q_ref.shape[1] // k_ref.shape[1]
    row = lax.broadcasted_iota(jnp.int32, (WINDOW, 2 * WINDOW), 0)
    col = lax.broadcasted_iota(jnp.int32, (WINDOW, 2 * WINDOW), 1)
    band = (col <= row + WINDOW) & (col > row)

    for kv in range(heads_kv):

        def block_step(n, carry, kv=kv):
            start = pl.multiple_of(n * WINDOW, WINDOW)
            keys = k_ext[pl.ds(start, 2 * WINDOW), kv * HD : (kv + 1) * HD]
            values = v_ext[pl.ds(start, 2 * WINDOW), kv * HD : (kv + 1) * HD]
            wide_q = q_ref[pl.ds(start, WINDOW), kv * grouping * HD : (kv + 1) * grouping * HD]
            visible = band & (col + (sp * length + start - WINDOW) >= 0)
            stacked = jnp.concatenate(
                [wide_q[:, g * HD : (g + 1) * HD] for g in range(grouping)], axis=0
            )
            scores = lax.dot_general(
                stacked, keys, (((1,), (1,)), ((), ())), preferred_element_type=jnp.float32
            ) * HD ** (-0.5)
            probs = []
            for g in range(grouping):
                sink = sink_ref[kv * grouping + g]
                part = jnp.where(visible, scores[g * WINDOW : (g + 1) * WINDOW], NEG_FILL)
                top = jnp.maximum(jnp.max(part, axis=-1, keepdims=True), sink)
                expo = jnp.exp(part - top)
                total = jnp.sum(expo, axis=-1, keepdims=True) + jnp.exp(sink - top)
                probs.append((expo / total).astype(jnp.bfloat16))
            result = jnp.dot(
                jnp.concatenate(probs, axis=0), values, preferred_element_type=jnp.float32
            ).astype(jnp.bfloat16)
            att[pl.ds(start, WINDOW), kv * grouping * HD : (kv + 1) * grouping * HD] = (
                jnp.concatenate(
                    [result[g * WINDOW : (g + 1) * WINDOW] for g in range(grouping)], axis=1
                )
            )
            return carry

        lax.fori_loop(0, length // WINDOW, block_step, 0)
        if kv < 3:
            ring_start(kv, 1)
    for m in range(min(heads_kv, 3), 3):
        ring_start(m, 1)

    columns = ow_ref.shape[1]
    tile = min(512, columns)

    def project(rows_start, target):
        def tile_step(t, carry):
            at = pl.multiple_of(t * tile, tile)
            target[:, pl.ds(at, tile)] = jnp.dot(
                att[pl.ds(rows_start, share)],
                ow_ref[:, pl.ds(at, tile)],
                preferred_element_type=jnp.float32,
            ).astype(jnp.bfloat16)
            return carry

        lax.fori_loop(0, columns // tile, tile_step, 0)

    project(pl.multiple_of(mate * share, share), snd)
    pair = begin(remote(snd, rcv, pair_s, pair_r, tp=mate))
    project(pl.multiple_of(tp * share, share), own)
    pair.wait_recv()
    band_rows = 32

    def norm_step(t, carry):
        at = pl.ds(pl.multiple_of(t * band_rows, band_rows), band_rows)
        proj = own[at].astype(jnp.float32) + rcv[at].astype(jnp.float32)
        middle = res_ref[at].astype(jnp.float32) + proj * row_scale(proj) * ga_ref[...]
        mid_ref[at] = middle
        nrm[at] = (middle * row_scale(middle) * gb_ref[...]).astype(jnp.bfloat16)
        return carry

    lax.fori_loop(0, share // band_rows, norm_step, 0)

    def slot(member, core):
        return rows_all.at[pl.ds(pl.multiple_of((member * 2 + core) * share, share), share)]

    mates = [begin(remote(nrm, slot(place, tp), mate_s.at[0], mate_r.at[0], tp=mate))]
    spread = {
        turn: begin(
            remote(
                nrm,
                slot(place, tp),
                rows_s.at[turn - 1],
                rows_r.at[turn - 1],
                sp=level * TEAM + team_peer(place, turn),
            )
        )
        for turn in (3, 1, 2)
    }
    mine = pltpu.make_async_copy(nrm, slot(place, tp), local_sem.at[3])
    mine.start()
    for step in range(2, last + 1):
        for m in range(3):
            ring_start(m, step)
    for turn in (1, 2, 3):
        spread[turn].wait_recv()
        block = slot(team_peer(place, turn), tp)
        mates.append(begin(remote(block, block, mate_s.at[turn], mate_r.at[turn], tp=mate)))
    mine.wait()
    for copy in mates:
        copy.wait_recv()
    for m in range(3):
        for side in range(2):
            ring_copies[m, last, side].wait_recv()
    for copy in sends:
        copy.wait_send()


def back_kernel(
    hid_ref, down_ref, mid_ref, gain_ref, out_ref, psnd, prcv, own, snd, rcv, ps, pr, ts, tr
):
    sp, tp = lax.axis_index("sp"), lax.axis_index("tp")
    level, place = sp // TEAM, sp % TEAM
    mate = 1 - tp
    share = mid_ref.shape[0]
    columns = down_ref.shape[1]
    tile = min(512, columns)
    greet(
        [{"sp": level * TEAM + team_peer(place, turn)} for turn in range(1, TEAM)]
        + [{"tp": mate}]
    )
    order = (3, 1, 2, 0)

    def product(turn, core, store):
        start = pl.multiple_of((team_peer(place, turn) * 2 + core) * share, share)

        def tile_step(t, carry):
            at = pl.ds(pl.multiple_of(t * tile, tile), tile)
            part = jnp.dot(
                hid_ref[pl.ds(start, share)], down_ref[:, at], preferred_element_type=jnp.float32
            )
            store(at, part)
            return carry

        lax.fori_loop(0, columns // tile, tile_step, 0)

    pairs, sends = [], []
    for i, turn in enumerate(order):

        def to_mate(at, part, i=i):
            psnd[i, :, at] = part.astype(jnp.bfloat16)

        product(turn, mate, to_mate)
        copy = remote(psnd.at[i], prcv.at[i], ps.at[i], pr.at[i], tp=mate)
        copy.start()
        pairs.append(copy)
    for i, turn in enumerate(order):
        pairs[i].wait_recv()

        def add_mate(at, part, i=i, turn=turn):
            total = part.astype(jnp.bfloat16).astype(jnp.float32) + prcv[i, :, at].astype(jnp.float32)
            if turn:
                snd[i, :, at] = total.astype(jnp.bfloat16)
            else:
                own[:, at] = total

        product(turn, tp, add_mate)
        if turn:
            copy = remote(
                snd.at[i],
                rcv.at[i],
                ts.at[i],
                tr.at[i],
                sp=level * TEAM + team_peer(place, turn),
            )
            copy.start()
            sends.append(copy)
    for copy in sends:
        copy.wait_recv()
    band_rows = 32

    def norm_step(t, carry):
        at = pl.ds(pl.multiple_of(t * band_rows, band_rows), band_rows)
        total = own[at]
        for i in range(TEAM - 1):
            total = total + rcv[i, at].astype(jnp.float32)
        out_ref[at] = (mid_ref[at] + total * row_scale(total) * gain_ref[...]).astype(out_ref.dtype)
        return carry

    lax.fori_loop(0, share // band_rows, norm_step, 0)
    for copy in pairs + sends:
        copy.wait_send()


def on_device_team(
    ring,
    queries,
    key_states,
    value_states,
    sink_logits,
    out_weight,
    residual,
    gain_attn,
    gain_before,
    gain_after,
    gate_weight,
    value_weight,
    gate_taps,
    value_taps,
    down_weight,
):
    length, width = queries.shape[0], residual.shape[1]
    share = residual.shape[0]
    deep, local_units = gate_weight.shape
    units = local_units // TEAM
    rows = length * TEAM
    vmem = pl.BlockSpec(memory_space=pltpu.VMEM)
    smem = pl.BlockSpec(memory_space=pltpu.SMEM)
    far = pl.BlockSpec(memory_space=pl.ANY)
    dma = pltpu.SemaphoreType.DMA
    bf16, f32 = jnp.bfloat16, jnp.float32

    def by_member(weight):
        return weight.reshape(deep, TEAM, units).transpose(1, 0, 2)

    steps = ring // 2
    rows_all, gate_all, value_all, down_all, middle = pl.pallas_call(
        functools.partial(front_kernel, ring),
        out_shape=(
            jax.ShapeDtypeStruct((rows, width), bf16),
            jax.ShapeDtypeStruct((width, units), bf16),
            jax.ShapeDtypeStruct((width, units), bf16),
            jax.ShapeDtypeStruct((units, width), bf16),
            jax.ShapeDtypeStruct((share, width), f32),
        ),
        in_specs=[vmem] * 3 + [smem] + [vmem] * 7,
        out_specs=(far, far, far, far, vmem),
        scratch_shapes=[
            pltpu.VMEM((length + WINDOW, key_states.shape[1]), bf16),
            pltpu.VMEM((length + WINDOW, key_states.shape[1]), bf16),
            pltpu.VMEM(queries.shape, bf16),
            pltpu.VMEM((share, width), bf16),
            pltpu.VMEM((share, width), bf16),
            pltpu.VMEM((share, width), bf16),
            pltpu.VMEM((share, width), bf16),
            dma((2,)),
            dma((2,)),
            dma((3, TEAM - 1)),
            dma((3, TEAM - 1)),
            dma((4,)),
            dma((3, steps, 2)),
            dma((3, steps, 2)),
            dma(()),
            dma(()),
            dma((TEAM - 1,)),
            dma((TEAM - 1,)),
            dma((TEAM,)),
            dma((TEAM,)),
        ],
        compiler_params=pltpu.CompilerParams(
            collective_id=0, has_side_effects=True, vmem_limit_bytes=VMEM_BYTES
        ),
        name="front",
    )(
        queries,
        key_states,
        value_states,
        sink_logits,
        out_weight,
        residual,
        gain_attn[None],
        gain_before[None],
        by_member(gate_weight),
        by_member(value_weight),
        down_weight,
    )
    gate_up = jnp.dot(rows_all, gate_all, preferred_element_type=f32).astype(bf16)
    value_up = jnp.dot(rows_all, value_all, preferred_element_type=f32).astype(bf16)
    reach = gate_taps.shape[0] - 1
    tails = passed_along(
        jnp.concatenate([gate_up[rows - reach :], value_up[rows - reach :]], axis=0), "sp", TEAM
    )
    first = lax.axis_index("sp") % TEAM * units
    gate_conv = causal_local(
        gate_up, tails[:reach], lax.dynamic_slice_in_dim(gate_taps, first, units, 1)
    )
    value_conv = causal_local(
        value_up, tails[reach:], lax.dynamic_slice_in_dim(value_taps, first, units, 1)
    )
    hidden = (jax.nn.silu(gate_conv) * value_conv).astype(bf16)
    return pl.pallas_call(
        back_kernel,
        out_shape=jax.ShapeDtypeStruct((share, width), bf16),
        in_specs=[vmem] * 4,
        out_specs=vmem,
        scratch_shapes=[
            pltpu.VMEM((TEAM, share, width), bf16),
            pltpu.VMEM((TEAM, share, width), bf16),
            pltpu.VMEM((share, width), f32),
            pltpu.VMEM((TEAM - 1, share, width), bf16),
            pltpu.VMEM((TEAM - 1, share, width), bf16),
            dma((TEAM,)),
            dma((TEAM,)),
            dma((TEAM - 1,)),
            dma((TEAM - 1,)),
        ],
        compiler_params=pltpu.CompilerParams(
            collective_id=1, has_side_effects=True, vmem_limit_bytes=VMEM_BYTES
        ),
        name="back",
    )(hidden, down_all, middle, gain_after[None])


def solution(mesh):
    in_specs = (
        P("sp", "tp"),
        P("sp", "tp"),
        P("sp", "tp"),
        P("tp"),
        P("tp", None),
        P(("sp", "tp"), None),
        P(),
        P(),
        P(),
        P("sp", "tp"),
        P("sp", "tp"),
        P(None, "tp"),
        P(None, "tp"),
        P("tp", "sp"),
    )
    out_specs = P(("sp", "tp"), None)
    members, cores = mesh.shape["sp"], mesh.shape["tp"]
    ring = members // TEAM

    def on_device(*args):
        units, wide = args[13].shape
        teams = cores == 2 and members % TEAM == 0 and ring >= 4 and ring % 2 == 0
        if teams and units % (TEAM * 16) == 0 and wide % 128 == 0:
            return on_device_team(ring, *args)
        return on_device_plain(*args)

    return jax.shard_map(
        on_device, mesh=mesh, in_specs=in_specs, out_specs=out_specs, check_vma=False
    )
```

```python
import functools

import jax
import jax.numpy as jnp
from jax import lax
from jax.experimental import pallas as pl
from jax.experimental.pallas import tpu as pltpu
from jax.sharding import PartitionSpec as P

HD = 64
WINDOW = 128
TEAM = 4


NEG_FILL = -1e30
MESH = pl.DeviceIdType.MESH
VMEM_BYTES = 60 * 1024 * 1024

def passed_along(block, axis, distance):
    devices = range(lax.axis_size(axis))
    route = [(i - distance, i) for i in devices if i - distance in devices]
    return lax.ppermute(block, axis, route)


def rms_scale(matrix):
    return matrix * lax.rsqrt(jnp.mean(matrix * matrix, axis=-1, keepdims=True) + 1e-06)


def attention_local(queries, key_states, value_states, sink_logits):
    length = queries.shape[0]
    blocks = length // WINDOW
    kv_local = key_states.shape[1] // HD
    grouping = queries.shape[1] // key_states.shape[1]
    earlier_keys, earlier_values = passed_along(
        (key_states[length - WINDOW :], value_states[length - WINDOW :]), "sp", 1
    )
    keys_ext = jnp.concatenate([earlier_keys, key_states], axis=0).reshape(
        blocks + 1, WINDOW, kv_local, HD
    )
    values_ext = jnp.concatenate([earlier_values, value_states], axis=0).reshape(
        blocks + 1, WINDOW, kv_local, HD
    )
    key_blocks = jnp.concatenate([keys_ext[:-1], keys_ext[1:]], axis=1)
    value_blocks = jnp.concatenate([values_ext[:-1], values_ext[1:]], axis=1)
    query_blocks = queries.reshape(blocks, WINDOW, kv_local, grouping, HD)
    offset = lax.axis_index("sp") * length
    qpos = (offset + jnp.arange(length, dtype=jnp.int32)).reshape(blocks, WINDOW)
    kpos = jnp.concatenate([qpos - WINDOW, qpos], axis=1)
    visible = (
        (kpos[:, None, :] <= qpos[:, :, None])
        & (qpos[:, :, None] - kpos[:, None, :] < WINDOW)
        & (kpos[:, None, :] >= 0)
    )
    scores = jnp.einsum(
        "nqhgd,nkhd->nhgqk", query_blocks, key_blocks, preferred_element_type=jnp.float32
    ) * HD ** (-0.5)
    scores = jnp.where(visible[:, None, None], scores, NEG_FILL)
    sink_col = sink_logits.reshape(kv_local, grouping)[None, :, :, None]
    top = jnp.maximum(jnp.max(scores, axis=-1), sink_col)
    expo = jnp.exp(scores - top[..., None])
    total = jnp.sum(expo, axis=-1) + jnp.exp(sink_col - top)
    probs = (expo / total[..., None]).astype(jnp.bfloat16)
    result = jnp.einsum(
        "nhgqk,nkhd->nqhgd", probs, value_blocks, preferred_element_type=jnp.float32
    )
    return result.astype(jnp.bfloat16).reshape(length, queries.shape[1])


def causal_local(upward, earlier, kernel):
    length = upward.shape[0]
    padded = jnp.concatenate([earlier, upward], axis=0).astype(jnp.float32)
    result = jnp.zeros(upward.shape, jnp.float32)
    for tap_index in range(kernel.shape[0]):
        result = result + kernel[tap_index][None, :] * padded[tap_index : tap_index + length]
    return result


def on_device_plain(
    queries,
    key_states,
    value_states,
    sink_logits,
    out_weight,
    residual,
    gain_attn,
    gain_before,
    gain_after,
    gate_weight,
    value_weight,
    gate_taps,
    value_taps,
    down_weight,
):
    length = queries.shape[0]
    attended = attention_local(queries, key_states, value_states, sink_logits)
    selected = attended
    attn_proj = lax.psum_scatter(
        jnp.dot(selected, out_weight, preferred_element_type=jnp.float32).astype(jnp.bfloat16),
        "tp",
        scatter_dimension=0,
        tiled=True,
    ).astype(jnp.float32)
    middle = residual.astype(jnp.float32) + rms_scale(attn_proj) * gain_attn
    normed = (rms_scale(middle) * gain_before).astype(jnp.bfloat16)
    whole_rows = lax.all_gather(normed, "tp", axis=0, tiled=True)
    gate_full, value_full = (
        lax.all_gather(gate_weight, "sp", axis=0, tiled=True),
        lax.all_gather(value_weight, "sp", axis=0, tiled=True),
    )
    gate_up = jnp.dot(whole_rows, gate_full, preferred_element_type=jnp.float32).astype(
        jnp.bfloat16
    )
    value_up = jnp.dot(whole_rows, value_full, preferred_element_type=jnp.float32).astype(
        jnp.bfloat16
    )
    reach = gate_taps.shape[0] - 1
    gate_before, value_before = passed_along(
        (gate_up[length - reach :], value_up[length - reach :]), "sp", 1
    )
    gate_conv = causal_local(gate_up, gate_before, gate_taps)
    value_conv = causal_local(value_up, value_before, value_taps)
    hidden = (jax.nn.silu(gate_conv) * value_conv).astype(jnp.bfloat16)
    down_whole = lax.all_gather(down_weight, "sp", axis=1, tiled=True)
    selected = hidden
    down = lax.psum_scatter(
        jnp.dot(selected, down_whole, preferred_element_type=jnp.float32).astype(jnp.bfloat16),
        "tp",
        scatter_dimension=0,
        tiled=True,
    ).astype(jnp.float32)
    return (middle + rms_scale(down) * gain_after).astype(jnp.bfloat16)


def team_peer(place, turn):
    low, high = place % 2, place // 2
    if turn & 1:
        low = 1 - low
    if turn & 2:
        high = 1 - high
    return high * 2 + low


def remote(src, dst, send, recv, **device):
    return pltpu.make_async_remote_copy(
        src_ref=src, dst_ref=dst, send_sem=send, recv_sem=recv, device_id=device, device_id_type=MESH
    )


def greet(devices):
    barrier = pltpu.get_barrier_semaphore()
    for device in devices:
        pl.semaphore_signal(barrier, inc=1, device_id=device, device_id_type=MESH)
    pl.semaphore_wait(barrier, len(devices))


def row_scale(block):
    return lax.rsqrt(jnp.mean(block * block, axis=-1, keepdims=True) + 1e-06)


def front_kernel(
    ring,
    q_ref,
    k_ref,
    v_ref,
    sink_ref,
    ow_ref,
    res_ref,
    ga_ref,
    gb_ref,
    gate_in,
    value_in,
    down_in,
    gate_taps,
    value_taps,
    hid_ref,
    down_all,
    mid_ref,
    rows_all,
    gate_all,
    value_all,
    gate_up,
    value_up,
    k_ext,
    v_ext,
    att,
    snd,
    rcv,
    own,
    nrm,
    halo_s,
    halo_r,
    trade_s,
    trade_r,
    local_sem,
    ring_s,
    ring_r,
    pair_s,
    pair_r,
    rows_s,
    rows_r,
    mate_s,
    mate_r,
    tail_s,
    tail_r,
):
    sp, tp = lax.axis_index("sp"), lax.axis_index("tp")
    members = ring * TEAM
    level, place = sp // TEAM, sp % TEAM
    up = (level + 1) % ring * TEAM + place
    down = (level + ring - 1) % ring * TEAM + place
    after, before = (sp + 1) % members, (sp + members - 1) % members
    mate = 1 - tp
    length = q_ref.shape[0]
    share = length // 2
    deep = gate_in.shape[1]
    units = gate_in.shape[2]
    wide = down_in.shape[1]
    sends = []

    greet(
        [{"sp": level * TEAM + team_peer(place, turn)} for turn in range(1, TEAM)]
        + [{"tp": mate}, {"sp": up}, {"sp": down}, {"sp": after}, {"sp": before}]
    )

    def begin(copy):
        copy.start()
        sends.append(copy)
        return copy

    halos = [
        begin(
            remote(
                ref.at[pl.ds(length - WINDOW, WINDOW)],
                ext.at[pl.ds(0, WINDOW)],
                halo_s.at[i],
                halo_r.at[i],
                sp=after,
            )
        )
        for i, (ref, ext) in enumerate(((k_ref, k_ext), (v_ref, v_ext)))
    ]

    def span(m, ref, start, size):
        if m < 2:
            return ref.at[pl.ds(pl.multiple_of(start * deep, deep), size * deep)]
        return ref.at[:, pl.ds(pl.multiple_of(start * wide, wide), size * wide)]

    def piece(m, member):
        if m < 2:
            return (gate_in, value_in)[m].at[member]
        return down_in.at[pl.ds(pl.multiple_of(member * units, units), units)]

    wholes = (gate_all, value_all, down_all)
    trades, locals_ = [], []
    for m in range(3):
        trades.append(
            [
                begin(
                    remote(
                        piece(m, team_peer(place, turn)),
                        span(m, wholes[m], sp, 1),
                        trade_s.at[m, turn - 1],
                        trade_r.at[m, turn - 1],
                        sp=level * TEAM + team_peer(place, turn),
                    )
                )
                for turn in (3, 1, 2)
            ]
        )
        copy = pltpu.make_async_copy(piece(m, place), span(m, wholes[m], sp, 1), local_sem.at[m])
        copy.start()
        locals_.append(copy)

    last = ring // 2
    ring_copies = {}

    def ring_start(m, step):
        if step == 1:
            locals_[m].wait()
            for copy in trades[m]:
                copy.wait_recv()
        for side, towards in ((0, up), (1, down)):
            if step > 1:
                ring_copies[m, step - 1, side].wait_recv()
            source = (level + ring - (step - 1)) % ring if side == 0 else (level + step - 1) % ring
            if step < last:
                block = span(m, wholes[m], source * TEAM, TEAM)
            else:
                block = span(m, wholes[m], source * TEAM + side * (TEAM // 2), TEAM // 2)
            sems = (ring_s.at[m, step - 1, side], ring_r.at[m, step - 1, side])
            ring_copies[m, step, side] = begin(remote(block, block, *sems, sp=towards))

    k_ext[pl.ds(WINDOW, length)] = k_ref[...]
    v_ext[pl.ds(WINDOW, length)] = v_ref[...]
    for copy in halos:
        copy.wait_recv()
    heads_kv = k_ref.shape[1] // HD
    grouping = q_ref.shape[1] // k_ref.shape[1]
    row = lax.broadcasted_iota(jnp.int32, (WINDOW, 2 * WINDOW), 0)
    col = lax.broadcasted_iota(jnp.int32, (WINDOW, 2 * WINDOW), 1)
    band = (col <= row + WINDOW) & (col > row)

    for kv in range(heads_kv):

        def block_step(n, carry, kv=kv):
            start = pl.multiple_of(n * WINDOW, WINDOW)
            keys = k_ext[pl.ds(start, 2 * WINDOW), kv * HD : (kv + 1) * HD]
            values = v_ext[pl.ds(start, 2 * WINDOW), kv * HD : (kv + 1) * HD]
            wide_q = q_ref[pl.ds(start, WINDOW), kv * grouping * HD : (kv + 1) * grouping * HD]
            visible = band & (col + (sp * length + start - WINDOW) >= 0)
            stacked = jnp.concatenate(
                [wide_q[:, g * HD : (g + 1) * HD] for g in range(grouping)], axis=0
            )
            scores = lax.dot_general(
                stacked, keys, (((1,), (1,)), ((), ())), preferred_element_type=jnp.float32
            ) * HD ** (-0.5)
            probs = []
            for g in range(grouping):
                sink = sink_ref[kv * grouping + g]
                part = jnp.where(visible, scores[g * WINDOW : (g + 1) * WINDOW], NEG_FILL)
                top = jnp.maximum(jnp.max(part, axis=-1, keepdims=True), sink)
                expo = jnp.exp(part - top)
                total = jnp.sum(expo, axis=-1, keepdims=True) + jnp.exp(sink - top)
                probs.append((expo / total).astype(jnp.bfloat16))
            result = jnp.dot(
                jnp.concatenate(probs, axis=0), values, preferred_element_type=jnp.float32
            ).astype(jnp.bfloat16)
            att[pl.ds(start, WINDOW), kv * grouping * HD : (kv + 1) * grouping * HD] = (
                jnp.concatenate(
                    [result[g * WINDOW : (g + 1) * WINDOW] for g in range(grouping)], axis=1
                )
            )
            return carry

        lax.fori_loop(0, length // WINDOW, block_step, 0)
        if kv < 2:
            ring_start(kv, 1)
    for m in range(min(heads_kv, 2), 2):
        ring_start(m, 1)

    columns = ow_ref.shape[1]
    tile = min(512, columns)

    def project(rows_start, target):
        def tile_step(t, carry):
            at = pl.multiple_of(t * tile, tile)
            target[:, pl.ds(at, tile)] = jnp.dot(
                att[pl.ds(rows_start, share)],
                ow_ref[:, pl.ds(at, tile)],
                preferred_element_type=jnp.float32,
            ).astype(jnp.bfloat16)
            return carry

        lax.fori_loop(0, columns // tile, tile_step, 0)

    project(pl.multiple_of(mate * share, share), snd)
    pair = begin(remote(snd, rcv, pair_s, pair_r, tp=mate))
    project(pl.multiple_of(tp * share, share), own)
    pair.wait_recv()
    band_rows = 32

    def norm_step(t, carry):
        at = pl.ds(pl.multiple_of(t * band_rows, band_rows), band_rows)
        proj = own[at].astype(jnp.float32) + rcv[at].astype(jnp.float32)
        middle = res_ref[at].astype(jnp.float32) + proj * row_scale(proj) * ga_ref[...]
        mid_ref[at] = middle
        nrm[at] = (middle * row_scale(middle) * gb_ref[...]).astype(jnp.bfloat16)
        return carry

    lax.fori_loop(0, share // band_rows, norm_step, 0)

    def slot(member, core):
        return rows_all.at[pl.ds(pl.multiple_of((member * 2 + core) * share, share), share)]

    mates = [begin(remote(nrm, slot(place, tp), mate_s.at[0], mate_r.at[0], tp=mate))]
    spread = {
        turn: begin(
            remote(
                nrm,
                slot(place, tp),
                rows_s.at[turn - 1],
                rows_r.at[turn - 1],
                sp=level * TEAM + team_peer(place, turn),
            )
        )
        for turn in (3, 1, 2)
    }
    mine = pltpu.make_async_copy(nrm, slot(place, tp), local_sem.at[3])
    mine.start()
    for step in range(2, last + 1):
        for m in range(2):
            ring_start(m, step)
    ring_start(2, 1)
    for turn in (1, 2, 3):
        spread[turn].wait_recv()
        block = slot(team_peer(place, turn), tp)
        mates.append(begin(remote(block, block, mate_s.at[turn], mate_r.at[turn], tp=mate)))
    mine.wait()
    for copy in mates:
        copy.wait_recv()

    rows = rows_all.shape[0]
    edge = gate_up.shape[0] - rows
    tails = []
    for m, result in enumerate((gate_up, value_up)):
        for side in range(2):
            ring_copies[m, last, side].wait_recv()

        def up_step(t, carry, m=m, result=result):
            at = pl.multiple_of(t * share, share)
            result[pl.ds(pl.multiple_of(at + edge, edge), share)] = jnp.dot(
                rows_all[pl.ds(at, share)], wholes[m][...], preferred_element_type=jnp.float32
            ).astype(jnp.bfloat16)
            return carry

        lax.fori_loop(0, rows // share, up_step, 0)
        tails.append(
            begin(
                remote(
                    result.at[pl.ds(rows, edge)],
                    result.at[pl.ds(0, edge)],
                    tail_s.at[m],
                    tail_r.at[m],
                    sp=up,
                )
            )
        )
    for step in range(2, last + 1):
        ring_start(2, step)
    for tail, result in zip(tails, (gate_up, value_up)):
        tail.wait_recv()
        result[pl.ds(0, edge)] = jnp.where(
            level > 0, result[pl.ds(0, edge)].astype(jnp.float32), 0.0
        ).astype(jnp.bfloat16)
    reach = gate_taps.shape[0] - 1
    conv_rows = 64

    def conv_step(t, carry):
        at = pl.multiple_of(t * conv_rows, conv_rows)

        def mixed(source, taps):
            padded = source[pl.ds(at, conv_rows + edge)].astype(jnp.float32)
            total = jnp.zeros((conv_rows, units), jnp.float32)
            for k in range(reach + 1):
                first = edge - reach + k
                total = total + taps[k : k + 1, :] * padded[first : first + conv_rows]
            return total

        gate = mixed(gate_up, gate_taps)
        value = mixed(value_up, value_taps)
        hid_ref[pl.ds(at, conv_rows)] = (gate / (1.0 + jnp.exp(-gate)) * value).astype(jnp.bfloat16)
        return carry

    lax.fori_loop(0, rows // conv_rows, conv_step, 0)
    for side in range(2):
        ring_copies[2, last, side].wait_recv()
    for copy in sends:
        copy.wait_send()


def back_kernel(
    hid_ref, down_ref, mid_ref, gain_ref, out_ref, psnd, prcv, own, snd, rcv, ps, pr, ts, tr
):
    sp, tp = lax.axis_index("sp"), lax.axis_index("tp")
    level, place = sp // TEAM, sp % TEAM
    mate = 1 - tp
    share = mid_ref.shape[0]
    columns = down_ref.shape[1]
    tile = min(512, columns)
    greet(
        [{"sp": level * TEAM + team_peer(place, turn)} for turn in range(1, TEAM)]
        + [{"tp": mate}]
    )
    order = (3, 1, 2, 0)

    def product(turn, core, store):
        start = pl.multiple_of((team_peer(place, turn) * 2 + core) * share, share)

        def tile_step(t, carry):
            at = pl.ds(pl.multiple_of(t * tile, tile), tile)
            part = jnp.dot(
                hid_ref[pl.ds(start, share)], down_ref[:, at], preferred_element_type=jnp.float32
            )
            store(at, part)
            return carry

        lax.fori_loop(0, columns // tile, tile_step, 0)

    pairs, sends = [], []
    for i, turn in enumerate(order):

        def to_mate(at, part, i=i):
            psnd[i, :, at] = part.astype(jnp.bfloat16)

        product(turn, mate, to_mate)
        copy = remote(psnd.at[i], prcv.at[i], ps.at[i], pr.at[i], tp=mate)
        copy.start()
        pairs.append(copy)
    for i, turn in enumerate(order):
        pairs[i].wait_recv()

        def add_mate(at, part, i=i, turn=turn):
            total = part.astype(jnp.bfloat16).astype(jnp.float32) + prcv[i, :, at].astype(jnp.float32)
            if turn:
                snd[i, :, at] = total.astype(jnp.bfloat16)
            else:
                own[:, at] = total

        product(turn, tp, add_mate)
        if turn:
            copy = remote(
                snd.at[i],
                rcv.at[i],
                ts.at[i],
                tr.at[i],
                sp=level * TEAM + team_peer(place, turn),
            )
            copy.start()
            sends.append(copy)
    for copy in sends:
        copy.wait_recv()
    band_rows = 32

    def norm_step(t, carry):
        at = pl.ds(pl.multiple_of(t * band_rows, band_rows), band_rows)
        total = own[at]
        for i in range(TEAM - 1):
            total = total + rcv[i, at].astype(jnp.float32)
        out_ref[at] = (mid_ref[at] + total * row_scale(total) * gain_ref[...]).astype(out_ref.dtype)
        return carry

    lax.fori_loop(0, share // band_rows, norm_step, 0)
    for copy in pairs + sends:
        copy.wait_send()


def on_device_team(
    ring,
    queries,
    key_states,
    value_states,
    sink_logits,
    out_weight,
    residual,
    gain_attn,
    gain_before,
    gain_after,
    gate_weight,
    value_weight,
    gate_taps,
    value_taps,
    down_weight,
):
    length, width = queries.shape[0], residual.shape[1]
    share = residual.shape[0]
    deep, local_units = gate_weight.shape
    units = local_units // TEAM
    rows = length * TEAM
    vmem = pl.BlockSpec(memory_space=pltpu.VMEM)
    smem = pl.BlockSpec(memory_space=pltpu.SMEM)
    far = pl.BlockSpec(memory_space=pl.ANY)
    dma = pltpu.SemaphoreType.DMA
    bf16, f32 = jnp.bfloat16, jnp.float32

    def by_member(weight):
        return weight.reshape(deep, TEAM, units).transpose(1, 0, 2)

    steps = ring // 2
    first = lax.axis_index("sp") % TEAM * units
    hidden, down_all, middle = pl.pallas_call(
        functools.partial(front_kernel, ring),
        out_shape=(
            jax.ShapeDtypeStruct((rows, units), bf16),
            jax.ShapeDtypeStruct((units, width), bf16),
            jax.ShapeDtypeStruct((share, width), f32),
        ),
        in_specs=[vmem] * 3 + [smem] + [vmem] * 9,
        out_specs=(vmem, far, vmem),
        scratch_shapes=[
            pltpu.VMEM((rows, width), bf16),
            pltpu.VMEM((width, units), bf16),
            pltpu.VMEM((width, units), bf16),
            pltpu.VMEM((rows + 16, units), bf16),
            pltpu.VMEM((rows + 16, units), bf16),
            pltpu.VMEM((length + WINDOW, key_states.shape[1]), bf16),
            pltpu.VMEM((length + WINDOW, key_states.shape[1]), bf16),
            pltpu.VMEM(queries.shape, bf16),
            pltpu.VMEM((share, width), bf16),
            pltpu.VMEM((share, width), bf16),
            pltpu.VMEM((share, width), bf16),
            pltpu.VMEM((share, width), bf16),
            dma((2,)),
            dma((2,)),
            dma((3, TEAM - 1)),
            dma((3, TEAM - 1)),
            dma((4,)),
            dma((3, steps, 2)),
            dma((3, steps, 2)),
            dma(()),
            dma(()),
            dma((TEAM - 1,)),
            dma((TEAM - 1,)),
            dma((TEAM,)),
            dma((TEAM,)),
            dma((2,)),
            dma((2,)),
        ],
        compiler_params=pltpu.CompilerParams(
            collective_id=0, has_side_effects=True, vmem_limit_bytes=VMEM_BYTES
        ),
        name="front",
    )(
        queries,
        key_states,
        value_states,
        sink_logits,
        out_weight,
        residual,
        gain_attn[None],
        gain_before[None],
        by_member(gate_weight),
        by_member(value_weight),
        down_weight,
        lax.dynamic_slice_in_dim(gate_taps, first, units, 1),
        lax.dynamic_slice_in_dim(value_taps, first, units, 1),
    )
    return pl.pallas_call(
        back_kernel,
        out_shape=jax.ShapeDtypeStruct((share, width), bf16),
        in_specs=[vmem] * 4,
        out_specs=vmem,
        scratch_shapes=[
            pltpu.VMEM((TEAM, share, width), bf16),
            pltpu.VMEM((TEAM, share, width), bf16),
            pltpu.VMEM((share, width), f32),
            pltpu.VMEM((TEAM - 1, share, width), bf16),
            pltpu.VMEM((TEAM - 1, share, width), bf16),
            dma((TEAM,)),
            dma((TEAM,)),
            dma((TEAM - 1,)),
            dma((TEAM - 1,)),
        ],
        compiler_params=pltpu.CompilerParams(
            collective_id=1, has_side_effects=True, vmem_limit_bytes=VMEM_BYTES
        ),
        name="back",
    )(hidden, down_all, middle, gain_after[None])


def solution(mesh):
    in_specs = (
        P("sp", "tp"),
        P("sp", "tp"),
        P("sp", "tp"),
        P("tp"),
        P("tp", None),
        P(("sp", "tp"), None),
        P(),
        P(),
        P(),
        P("sp", "tp"),
        P("sp", "tp"),
        P(None, "tp"),
        P(None, "tp"),
        P("tp", "sp"),
    )
    out_specs = P(("sp", "tp"), None)
    members, cores = mesh.shape["sp"], mesh.shape["tp"]
    ring = members // TEAM

    def on_device(*args):
        units, wide = args[13].shape
        teams = cores == 2 and members % TEAM == 0 and ring >= 4 and ring % 2 == 0
        if teams and units % (TEAM * 16) == 0 and wide % 128 == 0:
            return on_device_team(ring, *args)
        return on_device_plain(*args)

    return jax.shard_map(
        on_device, mesh=mesh, in_specs=in_specs, out_specs=out_specs, check_vma=False
    )
```
